32 devices in a mesh: sp: 4 (over y, x), tp: 8 (over z, core).
Axes of the slice: x: 2, y: 2, z: 4, core: 2. Of those that a mesh axis runs over, the one named last changes fastest.
Arguments:
- query_a: bfloat16 [512, 16, 256], P('sp', 'tp'), may hold values from -5.5 to 5.5
- key_a: bfloat16 [512, 16, 256], P('sp', 'tp'), may hold values from -5.5 to 5.5
- value_a: bfloat16 [512, 16, 256], P('sp', 'tp'), may hold values from -6 to 6
- query_b: bfloat16 [512, 16, 128], P('sp', 'tp'), may hold values from -5.5 to 5.5
- key_b: bfloat16 [512, 16, 128], P('sp', 'tp'), may hold values from -5.5 to 5.5
- value_b: bfloat16 [512, 16, 128], P('sp', 'tp'), may hold values from -6 to 6
- lambdas: float32 [2, 16], P(None, 'tp'), may hold values from 0.3 to 0.8
- gain_a: float32 [256], replicated, may hold values from 0.1 to 1.9
- gain_b: float32 [128], replicated, may hold values from 0.1 to 1.9
- out_a: bfloat16 [4096, 4096], P('tp'), may hold values from -0.078125 to 0.078125
- out_b: bfloat16 [2048, 4096], P('tp'), may hold values from -0.078125 to 0.078125
- residual: bfloat16 [512, 4096], P(('sp', 'tp')), may hold values from -6 to 6
- norm_gain: float32 [4096], replicated, may hold values from 0.1 to 1.9
- route_ids: int32 [512, 2], P(('sp', 'tp')), may hold values from 0 to 7, all different within a row; in each aligned block of 16 rows (0 to 15, 16 to 31, ...) at most 8 rows name the same one
- route_weights: float32 [512, 2], P(('sp', 'tp')), may hold values from 0.1 to 0.9
- w_gate: bfloat16 [8, 4096, 2048], P('sp', None, 'tp'), may hold values from -0.28125 to 0.28125
- w_up: bfloat16 [8, 4096, 2048], P('sp', None, 'tp'), may hold values from -0.28125 to 0.28125
- w_down: bfloat16 [8, 2048, 4096], P('sp', 'tp'), may hold values from -0.01977539 to 0.01977539
Outputs:
- result: bfloat16 [512, 4096], P(('sp', 'tp'))
The draws below stay inside these ranges and needn't reach their ends.
Inputs may be any that keep to these rules, and one draw needn't show every extreme that they name: `route_ids`: in the rows of one device each token names 2 different experts, no expert is named more than 8 times, a bound that some block reaches.
All inputs are finite; a program needn't handle non-finite values.
Results may differ from the reference program's by a relative error of at most 0.02.
Values may be sent and summed in bfloat16 or wider, within the bound.
A program may use at most 128 MiB of HBM per device.

```python
import math
import jax
import jax.numpy as jnp
import numpy as np
from jax import lax

D = 4096
HEADS = 16
DA = 128
DB = 64
VA = 256
VB = 128
F = 2048
TOPK = 2
ROWS = 16
EXPERTS = 8
TOK_DEV = 128
SEQ = 512
CAP = 8
N_SP = 4
N_TP = 8


def paired_maps(key, salt, width):
    base = jax.random.fold_in(key, salt)
    key_query, key_keys = jax.random.split(base, 2)
    shape = (SEQ, HEADS, 2 * width)
    queries = jnp.clip(1.3 * jax.random.normal(key_query, shape, jnp.float32), -5.5, 5.5)
    keys = jnp.clip(1.3 * jax.random.normal(key_keys, shape, jnp.float32), -5.5, 5.5)
    return (queries, keys)


def draw_query_a(key, part):
    return paired_maps(key, 101, DA)[0].astype(jnp.bfloat16)


def draw_key_a(key, part):
    return paired_maps(key, 101, DA)[1].astype(jnp.bfloat16)


def draw_query_b(key, part):
    return paired_maps(key, 202, DB)[0].astype(jnp.bfloat16)


def draw_key_b(key, part):
    return paired_maps(key, 202, DB)[1].astype(jnp.bfloat16)


def shard_levels(own_key, shape, cuts, least, high):
    loudness, own = 1.0, jax.random.fold_in(own_key, 6)
    for dim, blocks in cuts:
        heights = jnp.exp(jax.random.uniform(jax.random.fold_in(own, dim), (blocks,), jnp.float32, least / len(cuts), high / len(cuts)))
        loudness = loudness * jnp.repeat(heights, shape[dim] // blocks).reshape([-1 if axis == dim else 1 for axis in range(len(shape))])
    return loudness


def routed_block(rng, own, number, rows, count, top, bound, lean):
    sequence = jax.random.permutation(rng, count)
    packed, common = shares(count, rows * top, bound, lean, True), shares(count, rows * top, bound, lean, False)
    places = jnp.arange(count)

    def named(sizes, rotation):
        used = int((sizes > 0).sum())
        fixed = max(1, used // 4)
        shifted = fixed + (places - fixed + rotation * (used - fixed)) % max(1, count - fixed)
        return jnp.zeros((count,), jnp.int32).at[sequence[jnp.where(places < fixed, places, shifted)]].set(jnp.asarray(sizes, jnp.int32))

    sizes = jnp.where(number % 4 == 0, named(packed, number // 4), named(common, number - number // 4 - 1))
    mixed = jax.random.permutation(jax.random.fold_in(own, 3), count)
    donor, sink = mixed[0:count // 2 * 2:2], mixed[1:count // 2 * 2:2]
    margin = jnp.minimum(sizes[donor] - 1, bound - sizes[sink]) // 2
    margin = jnp.where((donor == sequence[0]) | (sink == sequence[0]) | (sizes[sink] == 0), 0, jnp.maximum(margin, 0))
    shifted = jax.random.randint(jax.random.fold_in(own, 4), (count // 2,), 0, 1 << 20) % (margin + 1)
    sizes = sizes.at[donor].add(-shifted).at[sink].add(shifted)
    items = jnp.searchsorted(jnp.cumsum(sizes), jnp.arange(rows * top), side="right").astype(jnp.int32)
    grid = items.reshape(top, rows).T
    grid = grid[jax.random.permutation(jax.random.fold_in(own, 1), rows)]
    rotation = jax.random.randint(jax.random.fold_in(own, 2), (rows, 1), 0, top)
    return jnp.take_along_axis(grid, (jnp.arange(top)[None, :] + rotation) % top, axis=1)


def shares(amount, total, limit, skew, full):
    loads = [(1 << 20) // math.isqrt(standing ** skew) + 1 for standing in range(1, amount + 1)]
    largest = limit if full else min(limit, max(-(-total // amount), total * loads[0] // sum(loads)))
    least = 1 if total - largest >= amount - 1 else 0
    given, spare = [largest] + [least] * (amount - 1), total - largest - least * (amount - 1)
    while spare > 0:
        candidates = [i for i in range(1, amount) if given[i] < largest] or [i for i in range(1, amount) if given[i] < limit]
        pool, budget = sum([loads[i] for i in candidates]), spare
        for i in candidates:
            more = min(limit - given[i], max(1, budget * loads[i] // pool), spare)
            given[i] = given[i] + more
            spare = spare - more
    return np.array(given)


def bell_draw(stream_key, dims, scale, most, cuts=(), kind=jnp.bfloat16):
    entries = scale * jax.random.normal(stream_key, dims, jnp.float32)
    if cuts:
        entries = entries * shard_levels(stream_key, dims, cuts, -0.22, 0.18)
    return jnp.clip(entries, -most, most).astype(kind)


def setup_inputs(seed: int = 0) -> dict:
    arg_keys = jax.random.split(jax.random.key(seed), 19)
    query_a = draw_query_a(jax.random.fold_in(arg_keys[18], 71), 0)
    key_a = draw_key_a(jax.random.fold_in(arg_keys[18], 71), 0)
    value_a = bell_draw(arg_keys[2], (SEQ, HEADS, VA), 1.0, 6.0, ((0, 4), (1, 8)))
    query_b = draw_query_b(jax.random.fold_in(arg_keys[18], 71), 0)
    key_b = draw_key_b(jax.random.fold_in(arg_keys[18], 71), 0)
    value_b = bell_draw(arg_keys[5], (SEQ, HEADS, VB), 1.0, 6.0, ((0, 4), (1, 8)))
    lambdas = jnp.clip(0.3 + 0.5 * jax.random.uniform(arg_keys[6], (2, HEADS), jnp.float32) ** shard_levels(arg_keys[6], (2, HEADS), ((1, 8),), -0.2, 0.2), 0.3, 0.8)
    gain_a = jnp.clip(1.0 + 0.18 * jax.random.normal(arg_keys[7], (VA,), jnp.float32), 0.1, 1.9)
    gain_b = jnp.clip(1.0 + 0.18 * jax.random.normal(arg_keys[8], (VB,), jnp.float32), 0.1, 1.9)
    out_a = bell_draw(arg_keys[9], (HEADS * VA, D), (HEADS * (VA + VB)) ** -0.5, 0.078125, ((0, 8),))
    out_b = bell_draw(arg_keys[10], (HEADS * VB, D), (HEADS * (VA + VB)) ** -0.5, 0.078125, ((0, 8),))
    residual = bell_draw(arg_keys[11], (SEQ, D), 1.0, 6.0, ((0, 32),))
    norm_gain = jnp.clip(1.0 + 0.18 * jax.random.normal(arg_keys[12], (D,), jnp.float32), 0.1, 1.9)
    route_ids_keys = jax.random.split(jax.random.fold_in(arg_keys[13], 1), SEQ // ROWS)
    route_ids_turns = jax.random.permutation(jax.random.fold_in(arg_keys[13], 3), SEQ // ROWS)
    route_ids = jax.vmap(lambda own, number: routed_block(jax.random.fold_in(arg_keys[13], 2), own, number, ROWS, EXPERTS, TOPK, CAP, 2))(route_ids_keys, route_ids_turns).reshape((SEQ, TOPK))
    route_weights = jnp.clip(0.1 + 0.79999997 * jax.random.uniform(arg_keys[14], (SEQ, TOPK), jnp.float32) ** shard_levels(arg_keys[14], (SEQ, TOPK), ((0, 32),), -0.2, 0.2), 0.1, 0.9)
    w_gate = bell_draw(arg_keys[15], (EXPERTS, D, F), (3.0 / D ** 0.5), 0.28125, ((0, 4), (2, 8)))
    w_up = bell_draw(arg_keys[16], (EXPERTS, D, F), (3.0 / D ** 0.5), 0.28125, ((0, 4), (2, 8)))
    w_down = bell_draw(arg_keys[17], (EXPERTS, F, D), (0.15 / F ** 0.5), 0.01977539, ((0, 4), (1, 8)))
    return dict(query_a=query_a, key_a=key_a, value_a=value_a, query_b=query_b, key_b=key_b, value_b=value_b, lambdas=lambdas, gain_a=gain_a, gain_b=gain_b, out_a=out_a, out_b=out_b, residual=residual, norm_gain=norm_gain, route_ids=route_ids, route_weights=route_weights, w_gate=w_gate, w_up=w_up, w_down=w_down)


EPSILON = 1e-06
LIMIT = 7.0
SLOPE = 1.702

def head_output(query_head, key_head, value_head, lambda_head, gain, width):
    scaling = width ** (-0.5)

    def block(query_block):
        heard = []
        for which in range(2):
            query_part = query_block[:, which * width:(which + 1) * width]
            key_part = key_head[:, which * width:(which + 1) * width]
            scores = jnp.dot(query_part, key_part.T, preferred_element_type=jnp.float32) * scaling
            highest = lax.optimization_barrier(jnp.max(scores, axis=1, keepdims=True))
            expo = jnp.exp(scores - highest)
            totals = lax.optimization_barrier(jnp.sum(expo, axis=1, keepdims=True))
            summed = jnp.dot(expo.astype(jnp.bfloat16), value_head, preferred_element_type=jnp.float32)
            heard.append(summed / totals)
        differ = heard[0] - lambda_head * heard[1]
        scaled = lax.rsqrt(lax.optimization_barrier(jnp.mean(differ * differ, axis=1, keepdims=True)) + EPSILON)
        return (differ * scaled * gain).astype(jnp.bfloat16)
    blocks = query_head.reshape(SEQ // TOK_DEV, TOK_DEV, 2 * width)
    return lax.map(block, blocks).reshape(SEQ, -1)

def group_output(queries, keys, values, lambda_row, gain, width):

    def one_head(items):
        return head_output(items[0], items[1], items[2], items[3], gain, width)
    heads = lax.map(one_head, (jnp.swapaxes(queries, 0, 1), jnp.swapaxes(keys, 0, 1), jnp.swapaxes(values, 0, 1), lambda_row))
    return jnp.swapaxes(heads, 0, 1).reshape(SEQ, -1)

def reference(query_a, key_a, value_a, query_b, key_b, value_b, lambdas, gain_a, gain_b, out_a, out_b, residual, norm_gain, route_ids, route_weights, w_gate, w_up, w_down):
    attended_a = group_output(query_a, key_a, value_a, lambdas[0], gain_a, DA)
    attended_b = group_output(query_b, key_b, value_b, lambdas[1], gain_b, DB)
    projected = jnp.dot(attended_a, out_a, preferred_element_type=jnp.float32) + jnp.dot(attended_b, out_b, preferred_element_type=jnp.float32)
    mixed = (residual.astype(jnp.float32) + projected).astype(jnp.bfloat16)
    widened = mixed.astype(jnp.float32)
    normed = (widened * lax.rsqrt(lax.optimization_barrier(jnp.mean(widened * widened, axis=1, keepdims=True)) + EPSILON) * norm_gain).astype(jnp.bfloat16)
    hidden_part = F // N_TP
    most_load = N_SP * N_TP * CAP

    def expert_step(running, expert):
        chosen = route_ids == expert
        weight = lax.optimization_barrier(jnp.sum(jnp.where(chosen, route_weights, jnp.float32(0.0)), axis=1))
        marked = jnp.any(chosen, axis=1)
        picked = jnp.nonzero(marked, size=most_load, fill_value=0)[0].astype(jnp.int32)
        counted = jnp.sum(marked.astype(jnp.int32))
        valid = jnp.arange(most_load, dtype=jnp.int32) < counted
        rows = normed[picked]
        gate = jnp.dot(rows, w_gate[expert], preferred_element_type=jnp.float32)
        upward = jnp.dot(rows, w_up[expert], preferred_element_type=jnp.float32)
        clamped = jnp.minimum(gate, LIMIT)
        active = (clamped * jax.nn.sigmoid(SLOPE * clamped) * (jnp.clip(upward, -LIMIT, LIMIT) + 1.0)).astype(jnp.bfloat16)
        blocks = active.astype(jnp.float32).reshape(most_load, N_TP, hidden_part)
        down = w_down[expert].astype(jnp.float32).reshape(N_TP, hidden_part, D)
        partial_value = jnp.einsum('rjf,jfd->jrd', blocks, down).astype(jnp.bfloat16)
        partial_value = lax.optimization_barrier(partial_value)
        expert_out = lax.optimization_barrier(jnp.sum(partial_value.astype(jnp.float32), axis=0)).astype(jnp.bfloat16)
        expert_out = lax.optimization_barrier(expert_out)
        scale_rows = jnp.where(valid, weight[picked], jnp.float32(0.0))
        running = running.at[picked].add(scale_rows[:, None] * expert_out.astype(jnp.float32))
        return (running, None)
    combined, _ = lax.scan(expert_step, jnp.zeros((SEQ, D), jnp.float32), jnp.arange(EXPERTS, dtype=jnp.int32))
    return (widened + combined).astype(jnp.bfloat16)
```

```python
import functools

import jax
import jax.numpy as jnp
from jax import lax
from jax.experimental import pallas as pl
from jax.experimental.pallas import tpu as pltpu
from jax.sharding import PartitionSpec as P

EPSILON = 1e-06
LIMIT = 7.0
SLOPE = 1.702
FLOOR = -1e30


def empty_state(heads_here, queries_here, value_width):
    maxima = jnp.full((2, heads_here, queries_here), FLOOR, jnp.float32)
    totals = jnp.zeros((2, heads_here, queries_here), jnp.float32)
    sums = jnp.zeros((2, heads_here, queries_here, value_width), jnp.float32)
    return (maxima, totals, sums)


def absorb_keys(states, queries, keys, values, width):
    maxima, totals, sums = states
    scaling = width ** (-0.5)
    new_maxima = []
    new_totals = []
    new_sums = []
    for which in range(2):
        query_part = queries[:, :, which * width : (which + 1) * width]
        key_part = keys[:, :, which * width : (which + 1) * width]
        scores = (
            jnp.einsum("qhd,khd->hqk", query_part, key_part, preferred_element_type=jnp.float32)
            * scaling
        )
        highest = jnp.maximum(maxima[which], jnp.max(scores, axis=2))
        expo = jnp.exp(scores - highest[:, :, None])
        factor = jnp.exp(maxima[which] - highest)
        new_totals.append(totals[which] * factor + jnp.sum(expo, axis=2))
        carried = jnp.einsum(
            "hqk,khv->hqv", expo.astype(jnp.bfloat16), values, preferred_element_type=jnp.float32
        )
        new_sums.append(sums[which] * factor[:, :, None] + carried)
        new_maxima.append(highest)
    return (jnp.stack(new_maxima), jnp.stack(new_totals), jnp.stack(new_sums))


def finish(states, lambda_row, gain):
    maxima, totals, sums = states
    heard = sums / totals[:, :, :, None]
    differ = heard[0] - lambda_row[:, None, None] * heard[1]
    scaled = lax.rsqrt(jnp.mean(differ * differ, axis=2, keepdims=True) + EPSILON)
    return (differ * scaled * gain).astype(jnp.bfloat16)


def gated_units(grid, w_gate, w_up):
    gate = jnp.einsum("necd,edf->necf", grid, w_gate, preferred_element_type=jnp.float32)
    upward = jnp.einsum("necd,edf->necf", grid, w_up, preferred_element_type=jnp.float32)
    clamped = jnp.minimum(gate, LIMIT)
    return (
        clamped * jax.nn.sigmoid(SLOPE * clamped) * (jnp.clip(upward, -LIMIT, LIMIT) + 1.0)
    ).astype(jnp.bfloat16)


def per_device_plain(
    query_a,
    key_a,
    value_a,
    query_b,
    key_b,
    value_b,
    lambdas,
    gain_a,
    gain_b,
    out_a,
    out_b,
    residual,
    norm_gain,
    route_ids,
    route_weights,
    w_gate,
    w_up,
    w_down,
):
    heads_here = query_a.shape[1]
    queries_here = query_a.shape[0]
    width_a = query_a.shape[2] // 2
    width_b = query_b.shape[2] // 2
    starting = (
        empty_state(heads_here, queries_here, value_a.shape[2]),
        empty_state(heads_here, queries_here, value_b.shape[2]),
    )
    keys_a = lax.all_gather(key_a, "sp", axis=0, tiled=True)
    values_a = lax.all_gather(value_a, "sp", axis=0, tiled=True)
    keys_b = lax.all_gather(key_b, "sp", axis=0, tiled=True)
    values_b = lax.all_gather(value_b, "sp", axis=0, tiled=True)
    state_a = absorb_keys(starting[0], query_a, keys_a, values_a, width_a)
    state_b = absorb_keys(starting[1], query_b, keys_b, values_b, width_b)
    attended_a = finish(state_a, lambdas[0], gain_a)
    attended_b = finish(state_b, lambdas[1], gain_b)
    model_width = out_a.shape[1]
    weights_a = out_a.reshape(heads_here, -1, model_width)
    weights_b = out_b.reshape(heads_here, -1, model_width)
    first = jnp.einsum("hqv,hvd->qd", attended_a, weights_a, preferred_element_type=jnp.float32)
    projected = lax.psum_scatter(
        (
            first
            + jnp.einsum("hqv,hvd->qd", attended_b, weights_b, preferred_element_type=jnp.float32)
        ).astype(jnp.bfloat16),
        "tp",
        scatter_dimension=0,
        tiled=True,
    ).astype(jnp.float32)
    mixed = (residual.astype(jnp.float32) + projected).astype(jnp.bfloat16)
    widened = mixed.astype(jnp.float32)
    normed = (
        widened
        * lax.rsqrt(jnp.mean(widened * widened, axis=1, keepdims=True) + EPSILON)
        * norm_gain
    ).astype(jnp.bfloat16)
    rows_here, chosen = route_ids.shape
    groups = lax.axis_size("sp")
    experts_here = w_gate.shape[0]
    experts_all = experts_here * groups
    capacity = 2 * rows_here * chosen // experts_all
    slots_here = experts_here * capacity
    flat_ids = route_ids.reshape(-1)
    onehot = (flat_ids[:, None] == jnp.arange(experts_all, dtype=jnp.int32)[None, :]).astype(
        jnp.int32
    )
    earlier = jnp.cumsum(onehot, axis=0) - onehot
    target = flat_ids * capacity + jnp.sum(earlier * onehot, axis=1)
    places = jnp.arange(experts_all * capacity, dtype=jnp.int32)
    layout = jnp.any(target.reshape(rows_here, chosen)[None, :, :] == places[:, None, None], axis=2)
    outgoing = jnp.dot(
        layout.astype(jnp.bfloat16), normed, preferred_element_type=jnp.float32
    ).astype(jnp.bfloat16)
    outgoing = outgoing.reshape(groups, slots_here, model_width)
    arrived = lax.all_to_all(outgoing, "sp", split_axis=0, concat_axis=0, tiled=True)
    pieces = lax.all_gather(arrived, "tp", axis=0, tiled=True)
    count = pieces.shape[0]
    grid = pieces.reshape(count, experts_here, capacity, model_width)
    active = gated_units(grid, w_gate, w_up)
    down = jnp.einsum("necf,efd->necd", active, w_down, preferred_element_type=jnp.float32)
    partial_value = down.astype(jnp.bfloat16).reshape(count, slots_here, model_width)
    totals = lax.psum_scatter(
        partial_value.astype(jnp.float32).astype(jnp.bfloat16),
        "tp",
        scatter_dimension=0,
        tiled=True,
    )
    summed = lax.all_to_all(totals, "sp", split_axis=0, concat_axis=0, tiled=True)
    results = summed.reshape(experts_all * capacity, model_width)
    picked = (
        jnp.take(results, target, axis=0)
        .reshape(rows_here, chosen, model_width)
        .astype(jnp.float32)
    )
    combined = jnp.sum(route_weights[:, :, None] * picked, axis=1)
    return (widened + combined).astype(jnp.bfloat16)


def layer_kernel(
    dims,
    kv_ref,
    q_ref,
    lam_ref,
    gain_a_ref,
    gain_b_ref,
    res_ref,
    norm_ref,
    route_ref,
    out_a_hbm,
    out_b_hbm,
    gate_hbm,
    up_hbm,
    down_hbm,
    o_ref,
    kv_all,
    out_a,
    out_b,
    w_gate,
    w_up,
    w_down,
    att_a,
    att_b,
    part,
    pair1,
    sum1,
    z1,
    mixed,
    x_all,
    act,
    contrib,
    pair2,
    red,
    sp2,
    z2s,
    z2,
    tot,
    loc_sem,
    kv_s,
    kv_r,
    p1_s,
    p1_r,
    z1_s,
    z1_r,
    gz_s,
    gz_r,
    gs_s,
    gs_r,
    gp_s,
    gp_r,
    p2_s,
    p2_r,
    s2_s,
    s2_r,
    z2_s,
    z2_r,
):
    n_sp, n_tp, heads, da, db, va, vb = dims
    nz = n_tp // 2
    f32, bf16 = jnp.float32, jnp.bfloat16
    sp = lax.axis_index("sp")
    tp = lax.axis_index("tp")
    z, core = tp // 2, tp % 2
    rows, width = res_ref.shape
    chunk = nz * 2 * rows
    experts_here, _, hidden = w_gate.shape
    experts_all = experts_here * n_sp

    def sp_at(e):
        return lax.rem(sp + e + n_sp, n_sp)

    def z_at(d):
        return lax.rem(z + d + nz, nz)

    partner = {"sp": sp, "tp": z * 2 + 1 - core}

    def to_sp(e):
        return {"sp": sp_at(e), "tp": tp}

    def to_z(d):
        return {"sp": sp, "tp": z_at(d) * 2 + core}

    def remote(src, dst, send, recv, device):
        return pltpu.make_async_remote_copy(
            src_ref=src,
            dst_ref=dst,
            send_sem=send,
            recv_sem=recv,
            device_id=device,
            device_id_type=pl.DeviceIdType.MESH,
        )

    def kv_copy(e):
        return remote(kv_ref, kv_all.at[sp], kv_s.at[e - 1], kv_r.at[e - 1], to_sp(e))

    def p1_copy(d):
        zz = z_at(d)
        return remote(part.at[1 - core, zz], pair1.at[zz], p1_s.at[d], p1_r.at[d], partner)

    def z1_copy(d):
        return remote(sum1.at[z_at(d)], z1.at[d - 1], z1_s.at[d - 1], z1_r.at[d - 1], to_z(d))

    def gz_copy(d):
        block = x_all.at[sp, z, core]
        return remote(block, block, gz_s.at[d - 1], gz_r.at[d - 1], to_z(d))

    def gs_copy(e, d):
        block = x_all.at[sp, z_at(-d), core]
        return remote(block, block, gs_s.at[e - 1, d], gs_r.at[e - 1, d], to_sp(e))

    def gp_copy(e, d):
        block = x_all.at[sp_at(-e), z_at(-d), core]
        return remote(block, block, gp_s.at[e, d], gp_r.at[e, d], partner)

    def p2_copy(e):
        return remote(contrib.at[e, 1 - core], pair2.at[e], p2_s.at[e], p2_r.at[e], partner)

    def s2_copy(e, d):
        zz = z_at(d)
        return remote(
            red.at[e, zz], sp2.at[e - 1, zz], s2_s.at[e - 1, d], s2_r.at[e - 1, d], to_sp(-e)
        )

    def z2_copy(d):
        return remote(z2s.at[d - 1], z2.at[d - 1], z2_s.at[d - 1], z2_r.at[d - 1], to_z(d))

    barrier = pltpu.get_barrier_semaphore()
    for e in range(1, n_sp):
        pl.semaphore_signal(
            barrier, inc=1, device_id=to_sp(e), device_id_type=pl.DeviceIdType.MESH
        )
    for d in range(1, nz):
        pl.semaphore_signal(barrier, inc=1, device_id=to_z(d), device_id_type=pl.DeviceIdType.MESH)
    pl.semaphore_signal(barrier, inc=1, device_id=partner, device_id_type=pl.DeviceIdType.MESH)
    pl.semaphore_wait(barrier, n_sp - 1 + nz - 1 + 1)

    for e in range(1, n_sp):
        kv_copy(e).start()
    loads = [
        pltpu.make_async_copy(src, dst, loc_sem.at[i])
        for i, (src, dst) in enumerate(
            (
                (kv_ref, kv_all.at[sp]),
                (out_a_hbm, out_a),
                (out_b_hbm, out_b),
                (gate_hbm, w_gate),
                (up_hbm, w_up),
                (down_hbm, w_down),
            )
        )
    ]
    for load in loads:
        load.start()
    loads[0].wait()
    for e in range(1, n_sp):
        kv_copy(e).wait_recv()

    positions = kv_all.shape[1] * n_sp

    def attend(q0, k0, v0, map_width, value_width, lam, gain):
        heard = []
        for which in range(2):
            if map_width % 128 == 0:
                query = q_ref[:, q0 + which * map_width : q0 + (which + 1) * map_width]
                keys = kv_all[:, :, k0 + which * map_width : k0 + (which + 1) * map_width]
            else:
                query = q_ref[:, q0 : q0 + 2 * map_width]
                lane = lax.broadcasted_iota(jnp.int32, query.shape, 1)
                inside = (lane >= which * map_width) & (lane < (which + 1) * map_width)
                query = jnp.where(inside, query.astype(f32), 0.0).astype(bf16)
                keys = kv_all[:, :, k0 : k0 + 2 * map_width]
            keys = keys.reshape(positions, keys.shape[2])
            scores = lax.dot_general(
                query, keys, (((1,), (1,)), ((), ())), preferred_element_type=f32
            ) * (map_width**-0.5)
            expo = jnp.exp(scores - jnp.max(scores, axis=1, keepdims=True))
            total = jnp.sum(expo, axis=1, keepdims=True)
            values = kv_all[:, :, v0 : v0 + value_width].reshape(positions, value_width)
            carried = jnp.dot(expo.astype(bf16), values, preferred_element_type=f32)
            heard.append(carried / total)
        differ = heard[0] - lam * heard[1]
        scaled = lax.rsqrt(jnp.mean(differ * differ, axis=1, keepdims=True) + EPSILON)
        return (differ * scaled * gain).astype(bf16)

    base_va = heads * 2 * da
    base_kb = base_va + heads * va
    base_vb = base_kb + heads * 2 * db
    for h in range(heads):
        att_a[:, h * va : (h + 1) * va] = attend(
            h * 2 * da, h * 2 * da, base_va + h * va, da, va, lam_ref[0, h], gain_a_ref[...]
        )
    for h in range(heads):
        att_b[:, h * vb : (h + 1) * vb] = attend(
            heads * 2 * da + h * 2 * db,
            base_kb + h * 2 * db,
            base_vb + h * vb,
            db,
            vb,
            lam_ref[1, h],
            gain_b_ref[...],
        )

    loads[1].wait()
    loads[2].wait()
    tile = 512

    @pl.loop(0, width // tile)
    def _(j):
        cols = pl.ds(pl.multiple_of(j * tile, tile), tile)
        value = jnp.dot(att_a[...], out_a[:, cols], preferred_element_type=f32) + jnp.dot(
            att_b[...], out_b[:, cols], preferred_element_type=f32
        )
        value = value.astype(bf16)
        for zz in range(nz):
            for c in range(2):
                r = (zz * 2 + c) * rows
                part[c, zz, :, cols] = value[r : r + rows]

    order = list(range(1, nz)) + [0]
    for d in order:
        p1_copy(d).start()
    for d in order:
        p1_copy(d).wait_recv()
        zz = z_at(d)
        both = part[core, zz].astype(f32) + pair1[zz].astype(f32)
        if d > 0:
            sum1[zz] = both.astype(bf16)
            z1_copy(d).start()
        else:
            tot[...] = both
    for d in range(1, nz):
        z1_copy(d).wait_recv()
        tot[...] += z1[d - 1].astype(f32)
    mix = (res_ref[...].astype(f32) + tot[...]).astype(bf16)
    mixed[...] = mix
    wide = mix.astype(f32)
    scaled = lax.rsqrt(jnp.mean(wide * wide, axis=1, keepdims=True) + EPSILON)
    x_all[sp, z, core, :, :width] = (wide * scaled * norm_ref[...]).astype(bf16)
    route = route_ref[...]
    high = route.astype(bf16)
    lane = lax.broadcasted_iota(jnp.int32, route.shape, 1)
    x_all[sp, z, core, :, width:] = jnp.where(
        lane < experts_all, high.astype(f32), route - high.astype(f32)
    ).astype(bf16)

    for d in range(1, nz):
        gz_copy(d).start()
    for e in range(1, n_sp):
        gs_copy(e, 0).start()
    gp_copy(0, 0).start()
    for d in range(1, nz):
        gz_copy(d).wait_recv()
        for e in range(1, n_sp):
            gs_copy(e, d).start()
        gp_copy(0, d).start()
    for load in loads[3:]:
        load.wait()

    @pl.loop(0, n_sp)
    def _(e):
        @pl.when(e > 0)
        def _():
            for d in range(nz):
                gs_copy(e, d).wait_recv()
                gp_copy(e, d).start()

        for d in range(nz):
            gp_copy(e, d).wait_recv()
        s = sp_at(-e)
        share = x_all[s, :, :, :, width:].reshape(chunk, route.shape[1]).astype(f32)
        lanes = lax.broadcasted_iota(jnp.int32, share.shape, 1)
        for j in range(experts_here):
            which = sp * experts_here + j
            weight = jnp.sum(
                jnp.where((lanes == which) | (lanes == which + experts_all), share, 0.0),
                axis=1,
                keepdims=True,
            )
            x = x_all[s, :, :, :, :width].reshape(chunk, width)
            gate = jnp.dot(x, w_gate[j], preferred_element_type=f32)
            upward = jnp.dot(x, w_up[j], preferred_element_type=f32)
            clamped = jnp.minimum(gate, LIMIT)
            active = (
                clamped * jax.nn.sigmoid(SLOPE * clamped) * (jnp.clip(upward, -LIMIT, LIMIT) + 1.0)
            )
            act[:, j * hidden : (j + 1) * hidden] = (active * weight).astype(bf16)

        @pl.loop(0, width // tile)
        def _(i):
            cols = pl.ds(pl.multiple_of(i * tile, tile), tile)
            rowsum = jnp.zeros((chunk, tile), f32)
            for j in range(experts_here):
                rowsum += jnp.dot(
                    act[:, j * hidden : (j + 1) * hidden],
                    w_down[j, :, cols],
                    preferred_element_type=f32,
                )
            value = rowsum.astype(bf16)
            for zz in range(nz):
                for c in range(2):
                    r = (zz * 2 + c) * rows
                    contrib[e, c, zz, :, cols] = value[r : r + rows]

        p2_copy(e).start()
        p2_copy(e).wait_recv()
        for d in order:
            zz = z_at(d)
            red[e, zz] = (contrib[e, core, zz].astype(f32) + pair2[e, zz].astype(f32)).astype(bf16)

            @pl.when(e > 0)
            def _():
                s2_copy(e, d).start()

    for d in order:
        zz = z_at(d)
        total = red[0, zz].astype(f32)
        for e in range(1, n_sp):
            s2_copy(e, d).wait_recv()
            total += sp2[e - 1, zz].astype(f32)
        if d > 0:
            z2s[d - 1] = total.astype(bf16)
            z2_copy(d).start()
        else:
            tot[...] = total
    for d in range(1, nz):
        z2_copy(d).wait_recv()
        tot[...] += z2[d - 1].astype(f32)
    o_ref[...] = (mixed[...].astype(f32) + tot[...]).astype(bf16)

    for e in range(1, n_sp):
        kv_copy(e).wait_send()
    for d in range(nz):
        p1_copy(d).wait_send()
    for d in range(1, nz):
        z1_copy(d).wait_send()
        gz_copy(d).wait_send()
        z2_copy(d).wait_send()
    for e in range(n_sp):
        p2_copy(e).wait_send()
        for d in range(nz):
            gp_copy(e, d).wait_send()
            if e > 0:
                gs_copy(e, d).wait_send()
                s2_copy(e, d).wait_send()


def per_device(
    n_sp,
    n_tp,
    query_a,
    key_a,
    value_a,
    query_b,
    key_b,
    value_b,
    lambdas,
    gain_a,
    gain_b,
    out_a,
    out_b,
    residual,
    norm_gain,
    route_ids,
    route_weights,
    w_gate,
    w_up,
    w_down,
):
    here, heads, _ = query_a.shape
    da, db = query_a.shape[2] // 2, query_b.shape[2] // 2
    va, vb = value_a.shape[2], value_b.shape[2]
    rows, width = residual.shape
    experts_here, _, hidden = w_gate.shape
    experts_all = experts_here * n_sp
    nz = n_tp // 2
    bf16, f32 = jnp.bfloat16, jnp.float32

    def flat(*arrays):
        return jnp.concatenate([a.reshape(here, -1) for a in arrays], axis=1)

    kv = flat(key_a, value_a, key_b, value_b)
    queries = flat(query_a, query_b)
    chosen = route_ids[:, :, None] == jnp.arange(experts_all, dtype=jnp.int32)
    dense = jnp.sum(jnp.where(chosen, route_weights[:, :, None], 0.0), axis=1)
    lanes = -(-2 * experts_all // 128) * 128
    route = jnp.concatenate(
        [dense, dense, jnp.zeros((rows, lanes - 2 * experts_all), f32)], axis=1
    )
    vmem = pl.BlockSpec(memory_space=pltpu.VMEM)
    hbm = pl.BlockSpec(memory_space=pl.ANY)
    sem = pltpu.SemaphoreType.DMA
    pairs = [(n_sp - 1,), (nz,), (nz - 1,), (nz - 1,), (n_sp - 1, nz), (n_sp, nz), (n_sp,)]
    pairs += [(n_sp - 1, nz), (nz - 1,)]
    scratch = [
        pltpu.VMEM((n_sp,) + kv.shape, bf16),
        pltpu.VMEM(out_a.shape, bf16),
        pltpu.VMEM(out_b.shape, bf16),
        pltpu.VMEM(w_gate.shape, bf16),
        pltpu.VMEM(w_up.shape, bf16),
        pltpu.VMEM(w_down.shape, bf16),
        pltpu.VMEM((here, heads * va), bf16),
        pltpu.VMEM((here, heads * vb), bf16),
        pltpu.VMEM((2, nz, rows, width), bf16),
        pltpu.VMEM((nz, rows, width), bf16),
        pltpu.VMEM((nz, rows, width), bf16),
        pltpu.VMEM((nz - 1, rows, width), bf16),
        pltpu.VMEM((rows, width), bf16),
        pltpu.VMEM((n_sp, nz, 2, rows, width + lanes), bf16),
        pltpu.VMEM((n_tp * rows, experts_here * hidden), bf16),
        pltpu.VMEM((n_sp, 2, nz, rows, width), bf16),
        pltpu.VMEM((n_sp, nz, rows, width), bf16),
        pltpu.VMEM((n_sp, nz, rows, width), bf16),
        pltpu.VMEM((n_sp - 1, nz, rows, width), bf16),
        pltpu.VMEM((nz - 1, rows, width), bf16),
        pltpu.VMEM((nz - 1, rows, width), bf16),
        pltpu.VMEM((rows, width), f32),
        sem((6,)),
    ]
    for shape in pairs:
        scratch += [sem(shape), sem(shape)]
    return pl.pallas_call(
        functools.partial(layer_kernel, (n_sp, n_tp, heads, da, db, va, vb)),
        out_shape=jax.ShapeDtypeStruct((rows, width), bf16),
        in_specs=[vmem, vmem, pl.BlockSpec(memory_space=pltpu.SMEM)] + [vmem] * 5 + [hbm] * 5,
        out_specs=vmem,
        scratch_shapes=scratch,
        compiler_params=pltpu.CompilerParams(
            collective_id=0, has_side_effects=True, vmem_limit_bytes=60 * 1024 * 1024
        ),
    )(
        kv,
        queries,
        lambdas,
        gain_a.reshape(1, -1),
        gain_b.reshape(1, -1),
        residual,
        norm_gain.reshape(1, -1),
        route,
        out_a,
        out_b,
        w_gate,
        w_up,
        w_down,
    )


def solution(mesh):
    in_specs = (
        P("sp", "tp", None),
        P("sp", "tp", None),
        P("sp", "tp", None),
        P("sp", "tp", None),
        P("sp", "tp", None),
        P("sp", "tp", None),
        P(None, "tp"),
        P(),
        P(),
        P("tp", None),
        P("tp", None),
        P(("sp", "tp"), None),
        P(),
        P(("sp", "tp"), None),
        P(("sp", "tp"), None),
        P("sp", None, "tp"),
        P("sp", None, "tp"),
        P("sp", "tp", None),
    )
    out_specs = P(("sp", "tp"), None)
    n_sp, n_tp = mesh.shape["sp"], mesh.shape["tp"]
    fits = n_tp % 2 == 0 and n_sp * n_tp <= 32
    body = functools.partial(per_device, n_sp, n_tp) if fits else per_device_plain
    return jax.shard_map(
        body, mesh=mesh, in_specs=in_specs, out_specs=out_specs, check_vma=False
    )
```

```python
import functools

import jax
import jax.numpy as jnp
from jax import lax
from jax.experimental import pallas as pl
from jax.experimental.pallas import tpu as pltpu
from jax.sharding import PartitionSpec as P

EPSILON = 1e-06
LIMIT = 7.0
SLOPE = 1.702
FLOOR = -1e30


def empty_state(heads_here, queries_here, value_width):
    maxima = jnp.full((2, heads_here, queries_here), FLOOR, jnp.float32)
    totals = jnp.zeros((2, heads_here, queries_here), jnp.float32)
    sums = jnp.zeros((2, heads_here, queries_here, value_width), jnp.float32)
    return (maxima, totals, sums)


def absorb_keys(states, queries, keys, values, width):
    maxima, totals, sums = states
    scaling = width ** (-0.5)
    new_maxima = []
    new_totals = []
    new_sums = []
    for which in range(2):
        query_part = queries[:, :, which * width : (which + 1) * width]
        key_part = keys[:, :, which * width : (which + 1) * width]
        scores = (
            jnp.einsum("qhd,khd->hqk", query_part, key_part, preferred_element_type=jnp.float32)
            * scaling
        )
        highest = jnp.maximum(maxima[which], jnp.max(scores, axis=2))
        expo = jnp.exp(scores - highest[:, :, None])
        factor = jnp.exp(maxima[which] - highest)
        new_totals.append(totals[which] * factor + jnp.sum(expo, axis=2))
        carried = jnp.einsum(
            "hqk,khv->hqv", expo.astype(jnp.bfloat16), values, preferred_element_type=jnp.float32
        )
        new_sums.append(sums[which] * factor[:, :, None] + carried)
        new_maxima.append(highest)
    return (jnp.stack(new_maxima), jnp.stack(new_totals), jnp.stack(new_sums))


def finish(states, lambda_row, gain):
    maxima, totals, sums = states
    heard = sums / totals[:, :, :, None]
    differ = heard[0] - lambda_row[:, None, None] * heard[1]
    scaled = lax.rsqrt(jnp.mean(differ * differ, axis=2, keepdims=True) + EPSILON)
    return (differ * scaled * gain).astype(jnp.bfloat16)


def gated_units(grid, w_gate, w_up):
    gate = jnp.einsum("necd,edf->necf", grid, w_gate, preferred_element_type=jnp.float32)
    upward = jnp.einsum("necd,edf->necf", grid, w_up, preferred_element_type=jnp.float32)
    clamped = jnp.minimum(gate, LIMIT)
    return (
        clamped * jax.nn.sigmoid(SLOPE * clamped) * (jnp.clip(upward, -LIMIT, LIMIT) + 1.0)
    ).astype(jnp.bfloat16)


def per_device_plain(
    query_a,
    key_a,
    value_a,
    query_b,
    key_b,
    value_b,
    lambdas,
    gain_a,
    gain_b,
    out_a,
    out_b,
    residual,
    norm_gain,
    route_ids,
    route_weights,
    w_gate,
    w_up,
    w_down,
):
    heads_here = query_a.shape[1]
    queries_here = query_a.shape[0]
    width_a = query_a.shape[2] // 2
    width_b = query_b.shape[2] // 2
    starting = (
        empty_state(heads_here, queries_here, value_a.shape[2]),
        empty_state(heads_here, queries_here, value_b.shape[2]),
    )
    keys_a = lax.all_gather(key_a, "sp", axis=0, tiled=True)
    values_a = lax.all_gather(value_a, "sp", axis=0, tiled=True)
    keys_b = lax.all_gather(key_b, "sp", axis=0, tiled=True)
    values_b = lax.all_gather(value_b, "sp", axis=0, tiled=True)
    state_a = absorb_keys(starting[0], query_a, keys_a, values_a, width_a)
    state_b = absorb_keys(starting[1], query_b, keys_b, values_b, width_b)
    attended_a = finish(state_a, lambdas[0], gain_a)
    attended_b = finish(state_b, lambdas[1], gain_b)
    model_width = out_a.shape[1]
    weights_a = out_a.reshape(heads_here, -1, model_width)
    weights_b = out_b.reshape(heads_here, -1, model_width)
    first = jnp.einsum("hqv,hvd->qd", attended_a, weights_a, preferred_element_type=jnp.float32)
    projected = lax.psum_scatter(
        (
            first
            + jnp.einsum("hqv,hvd->qd", attended_b, weights_b, preferred_element_type=jnp.float32)
        ).astype(jnp.bfloat16),
        "tp",
        scatter_dimension=0,
        tiled=True,
    ).astype(jnp.float32)
    mixed = (residual.astype(jnp.float32) + projected).astype(jnp.bfloat16)
    widened = mixed.astype(jnp.float32)
    normed = (
        widened
        * lax.rsqrt(jnp.mean(widened * widened, axis=1, keepdims=True) + EPSILON)
        * norm_gain
    ).astype(jnp.bfloat16)
    rows_here, chosen = route_ids.shape
    groups = lax.axis_size("sp")
    experts_here = w_gate.shape[0]
    experts_all = experts_here * groups
    capacity = 2 * rows_here * chosen // experts_all
    slots_here = experts_here * capacity
    flat_ids = route_ids.reshape(-1)
    onehot = (flat_ids[:, None] == jnp.arange(experts_all, dtype=jnp.int32)[None, :]).astype(
        jnp.int32
    )
    earlier = jnp.cumsum(onehot, axis=0) - onehot
    target = flat_ids * capacity + jnp.sum(earlier * onehot, axis=1)
    places = jnp.arange(experts_all * capacity, dtype=jnp.int32)
    layout = jnp.any(target.reshape(rows_here, chosen)[None, :, :] == places[:, None, None], axis=2)
    outgoing = jnp.dot(
        layout.astype(jnp.bfloat16), normed, preferred_element_type=jnp.float32
    ).astype(jnp.bfloat16)
    outgoing = outgoing.reshape(groups, slots_here, model_width)
    arrived = lax.all_to_all(outgoing, "sp", split_axis=0, concat_axis=0, tiled=True)
    pieces = lax.all_gather(arrived, "tp", axis=0, tiled=True)
    count = pieces.shape[0]
    grid = pieces.reshape(count, experts_here, capacity, model_width)
    active = gated_units(grid, w_gate, w_up)
    down = jnp.einsum("necf,efd->necd", active, w_down, preferred_element_type=jnp.float32)
    partial_value = down.astype(jnp.bfloat16).reshape(count, slots_here, model_width)
    totals = lax.psum_scatter(
        partial_value.astype(jnp.float32).astype(jnp.bfloat16),
        "tp",
        scatter_dimension=0,
        tiled=True,
    )
    summed = lax.all_to_all(totals, "sp", split_axis=0, concat_axis=0, tiled=True)
    results = summed.reshape(experts_all * capacity, model_width)
    picked = (
        jnp.take(results, target, axis=0)
        .reshape(rows_here, chosen, model_width)
        .astype(jnp.float32)
    )
    combined = jnp.sum(route_weights[:, :, None] * picked, axis=1)
    return (widened + combined).astype(jnp.bfloat16)


def layer_kernel(
    dims,
    kv_ref,
    q_ref,
    lam_ref,
    gain_a_ref,
    gain_b_ref,
    res_ref,
    norm_ref,
    route_ref,
    out_a_hbm,
    out_b_hbm,
    gate_hbm,
    up_hbm,
    down_hbm,
    o_ref,
    kv_all,
    out_a,
    out_b,
    w_gate,
    w_up,
    w_down,
    att_a,
    att_b,
    part,
    pair1,
    sum1,
    z1,
    mixed,
    x_all,
    act,
    contrib,
    pair2,
    red,
    sp2,
    z2s,
    z2,
    tot,
    loc_sem,
    kv_s,
    kv_r,
    p1_s,
    p1_r,
    z1_s,
    z1_r,
    gz_s,
    gz_r,
    gs_s,
    gs_r,
    gp_s,
    gp_r,
    p2_s,
    p2_r,
    s2_s,
    s2_r,
    z2_s,
    z2_r,
):
    n_sp, n_tp, heads, da, db, va, vb = dims
    nz = n_tp // 2
    f32, bf16 = jnp.float32, jnp.bfloat16
    sp = lax.axis_index("sp")
    tp = lax.axis_index("tp")
    z, core = tp // 2, tp % 2
    rows, width = res_ref.shape
    chunk = n_sp * 2 * rows
    experts_here, _, hidden = w_gate.shape
    experts_all = experts_here * n_sp

    def sp_at(e):
        return lax.rem(sp + e + n_sp, n_sp)

    def z_at(d):
        return lax.rem(z + d + nz, nz)

    partner = {"sp": sp, "tp": z * 2 + 1 - core}

    def to_sp(e):
        return {"sp": sp_at(e), "tp": tp}

    def to_z(d):
        return {"sp": sp, "tp": z_at(d) * 2 + core}

    def remote(src, dst, send, recv, device):
        return pltpu.make_async_remote_copy(
            src_ref=src,
            dst_ref=dst,
            send_sem=send,
            recv_sem=recv,
            device_id=device,
            device_id_type=pl.DeviceIdType.MESH,
        )

    x_next = sp + 1 - 2 * (sp % 2)
    y_next = lax.rem(sp + 2, n_sp)

    def kv_copy(i):
        owner, target, half = (
            (sp, x_next, 0),
            (sp, y_next, 1),
            (sp, x_next, 1),
            (sp, y_next, 0),
            (x_next, y_next, 0),
            (y_next, x_next, 1),
        )[i]
        size = kv_ref.shape[0] // 2
        part_rows = pl.ds(half * size, size)
        place = kv_all.at[owner, part_rows]
        source = kv_ref.at[part_rows] if i < 4 else place
        return remote(source, place, kv_s.at[i], kv_r.at[i], {"sp": target, "tp": tp})

    def p1_copy(d):
        zz = z_at(d)
        return remote(part.at[1 - core, zz], pair1.at[zz], p1_s.at[d], p1_r.at[d], partner)

    def z1_copy(d):
        return remote(sum1.at[z_at(d)], z1.at[d - 1], z1_s.at[d - 1], z1_r.at[d - 1], to_z(d))

    def gz_copy(d):
        block = x_all.at[z, sp, core]
        return remote(block, block, gz_s.at[d - 1], gz_r.at[d - 1], to_z(d))

    def gs_copy(e, d):
        block = x_all.at[z_at(-d), sp, core]
        return remote(block, block, gs_s.at[e - 1, d], gs_r.at[e - 1, d], to_sp(e))

    def gp_copy(e, d):
        block = x_all.at[z_at(-d), sp_at(-e), core]
        return remote(block, block, gp_s.at[e, d], gp_r.at[e, d], partner)

    def p2_copy(d):
        return remote(contrib.at[d, 1 - core], pair2.at[d], p2_s.at[d], p2_r.at[d], partner)

    def s2_copy(e, d):
        return remote(
            red.at[d, sp_at(e)], sp2.at[e - 1, d], s2_s.at[e - 1, d], s2_r.at[e - 1, d], to_sp(e)
        )

    def z2_copy(d):
        return remote(z2s.at[d - 1], z2.at[d - 1], z2_s.at[d - 1], z2_r.at[d - 1], to_z(-d))

    barrier = pltpu.get_barrier_semaphore()
    for e in range(1, n_sp):
        pl.semaphore_signal(
            barrier, inc=1, device_id=to_sp(e), device_id_type=pl.DeviceIdType.MESH
        )
    for d in range(1, nz):
        pl.semaphore_signal(barrier, inc=1, device_id=to_z(d), device_id_type=pl.DeviceIdType.MESH)
    pl.semaphore_signal(barrier, inc=1, device_id=partner, device_id_type=pl.DeviceIdType.MESH)
    pl.semaphore_wait(barrier, n_sp - 1 + nz - 1 + 1)

    for i in range(4):
        kv_copy(i).start()
    loads = [
        pltpu.make_async_copy(src, dst, loc_sem.at[i])
        for i, (src, dst) in enumerate(
            (
                (kv_ref, kv_all.at[sp]),
                (out_a_hbm, out_a),
                (out_b_hbm, out_b),
                (gate_hbm, w_gate),
                (up_hbm, w_up),
                (down_hbm, w_down),
            )
        )
    ]
    for load in loads:
        load.start()
    loads[0].wait()
    for i in range(2):
        kv_copy(i).wait_recv()
        kv_copy(4 + i).start()
    for i in range(2, 6):
        kv_copy(i).wait_recv()

    positions = kv_all.shape[1] * n_sp

    def attend(q0, k0, v0, map_width, value_width, lam, gain):
        heard = []
        for which in range(2):
            if map_width % 128 == 0:
                query = q_ref[:, q0 + which * map_width : q0 + (which + 1) * map_width]
                keys = kv_all[:, :, k0 + which * map_width : k0 + (which + 1) * map_width]
            else:
                query = q_ref[:, q0 : q0 + 2 * map_width]
                lane = lax.broadcasted_iota(jnp.int32, query.shape, 1)
                inside = (lane >= which * map_width) & (lane < (which + 1) * map_width)
                query = jnp.where(inside, query.astype(f32), 0.0).astype(bf16)
                keys = kv_all[:, :, k0 : k0 + 2 * map_width]
            keys = keys.reshape(positions, keys.shape[2])
            scores = lax.dot_general(
                query, keys, (((1,), (1,)), ((), ())), preferred_element_type=f32
            ) * (map_width**-0.5)
            expo = jnp.exp(scores - jnp.max(scores, axis=1, keepdims=True))
            total = jnp.sum(expo, axis=1, keepdims=True)
            values = kv_all[:, :, v0 : v0 + value_width].reshape(positions, value_width)
            carried = jnp.dot(expo.astype(bf16), values, preferred_element_type=f32)
            heard.append(carried / total)
        differ = heard[0] - lam * heard[1]
        scaled = lax.rsqrt(jnp.mean(differ * differ, axis=1, keepdims=True) + EPSILON)
        return (differ * scaled * gain).astype(bf16)

    base_va = heads * 2 * da
    base_kb = base_va + heads * va
    base_vb = base_kb + heads * 2 * db
    for h in range(heads):
        att_a[:, h * va : (h + 1) * va] = attend(
            h * 2 * da, h * 2 * da, base_va + h * va, da, va, lam_ref[0, h], gain_a_ref[...]
        )
    for h in range(heads):
        att_b[:, h * vb : (h + 1) * vb] = attend(
            heads * 2 * da + h * 2 * db,
            base_kb + h * 2 * db,
            base_vb + h * vb,
            db,
            vb,
            lam_ref[1, h],
            gain_b_ref[...],
        )

    loads[1].wait()
    loads[2].wait()
    tile = 512

    @pl.loop(0, width // tile)
    def _(j):
        cols = pl.ds(pl.multiple_of(j * tile, tile), tile)
        value = jnp.dot(att_a[...], out_a[:, cols], preferred_element_type=f32) + jnp.dot(
            att_b[...], out_b[:, cols], preferred_element_type=f32
        )
        value = value.astype(bf16)
        for zz in range(nz):
            for c in range(2):
                r = (zz * 2 + c) * rows
                part[c, zz, :, cols] = value[r : r + rows]

    order = list(range(1, nz)) + [0]
    for d in order:
        p1_copy(d).start()
    for d in order:
        p1_copy(d).wait_recv()
        zz = z_at(d)
        both = part[core, zz].astype(f32) + pair1[zz].astype(f32)
        if d > 0:
            sum1[zz] = both.astype(bf16)
            z1_copy(d).start()
        else:
            tot[...] = both
    for d in range(1, nz):
        z1_copy(d).wait_recv()
        tot[...] += z1[d - 1].astype(f32)
    mix = (res_ref[...].astype(f32) + tot[...]).astype(bf16)
    mixed[...] = mix
    wide = mix.astype(f32)
    scaled = lax.rsqrt(jnp.mean(wide * wide, axis=1, keepdims=True) + EPSILON)
    x_all[z, sp, core, :, :width] = (wide * scaled * norm_ref[...]).astype(bf16)
    route = route_ref[...]
    high = route.astype(bf16)
    lane = lax.broadcasted_iota(jnp.int32, route.shape, 1)
    x_all[z, sp, core, :, width:] = jnp.where(
        lane < experts_all, high.astype(f32), route - high.astype(f32)
    ).astype(bf16)

    for d in range(1, nz):
        gz_copy(d).start()
    for e in range(1, n_sp):
        gs_copy(e, 0).start()
    gp_copy(0, 0).start()
    for load in loads[3:]:
        load.wait()

    def settle(d):
        total = red[d, sp].astype(f32)
        for e in range(1, n_sp):
            s2_copy(e, d).wait_recv()
            total += sp2[e - 1, d].astype(f32)

        @pl.when(d > 0)
        def _():
            z2s[d - 1] = total.astype(bf16)
            z2_copy(d).start()

        @pl.when(d == 0)
        def _():
            tot[...] = total

    @pl.loop(0, nz)
    def _(d):
        @pl.when(d + 1 < nz)
        def _():
            gz_copy(d + 1).wait_recv()
            for e in range(1, n_sp):
                gs_copy(e, d + 1).start()
            gp_copy(0, d + 1).start()

        for e in range(1, n_sp):
            gs_copy(e, d).wait_recv()
            gp_copy(e, d).start()
        for e in range(n_sp):
            gp_copy(e, d).wait_recv()
        zz = z_at(-d)
        share = x_all[zz, :, :, :, width:].reshape(chunk, route.shape[1]).astype(f32)
        lanes = lax.broadcasted_iota(jnp.int32, share.shape, 1)
        for j in range(experts_here):
            which = sp * experts_here + j
            weight = jnp.sum(
                jnp.where((lanes == which) | (lanes == which + experts_all), share, 0.0),
                axis=1,
                keepdims=True,
            )
            x = x_all[zz, :, :, :, :width].reshape(chunk, width)
            gate = jnp.dot(x, w_gate[j], preferred_element_type=f32)
            upward = jnp.dot(x, w_up[j], preferred_element_type=f32)
            clamped = jnp.minimum(gate, LIMIT)
            active = (
                clamped * jax.nn.sigmoid(SLOPE * clamped) * (jnp.clip(upward, -LIMIT, LIMIT) + 1.0)
            )
            act[:, j * hidden : (j + 1) * hidden] = (active * weight).astype(bf16)

        @pl.loop(0, width // tile)
        def _(i):
            cols = pl.ds(pl.multiple_of(i * tile, tile), tile)
            rowsum = jnp.zeros((chunk, tile), f32)
            for j in range(experts_here):
                rowsum += jnp.dot(
                    act[:, j * hidden : (j + 1) * hidden],
                    w_down[j, :, cols],
                    preferred_element_type=f32,
                )
            value = rowsum.astype(bf16)
            for s in range(n_sp):
                for c in range(2):
                    r = (s * 2 + c) * rows
                    contrib[d, c, s, :, cols] = value[r : r + rows]

        p2_copy(d).start()
        p2_copy(d).wait_recv()
        for e in list(range(1, n_sp)) + [0]:
            s = sp_at(e)
            red[d, s] = (contrib[d, core, s].astype(f32) + pair2[d, s].astype(f32)).astype(bf16)
            if e > 0:
                s2_copy(e, d).start()

        @pl.when(d > 0)
        def _():
            settle(d - 1)

    settle(nz - 1)
    for d in range(1, nz):
        z2_copy(d).wait_recv()
        tot[...] += z2[d - 1].astype(f32)
    o_ref[...] = (mixed[...].astype(f32) + tot[...]).astype(bf16)

    for i in range(6):
        kv_copy(i).wait_send()
    for d in range(nz):
        p1_copy(d).wait_send()
    for d in range(1, nz):
        z1_copy(d).wait_send()
        gz_copy(d).wait_send()
        z2_copy(d).wait_send()
    for d in range(nz):
        p2_copy(d).wait_send()
        for e in range(n_sp):
            gp_copy(e, d).wait_send()
            if e > 0:
                gs_copy(e, d).wait_send()
                s2_copy(e, d).wait_send()


def per_device(
    n_sp,
    n_tp,
    query_a,
    key_a,
    value_a,
    query_b,
    key_b,
    value_b,
    lambdas,
    gain_a,
    gain_b,
    out_a,
    out_b,
    residual,
    norm_gain,
    route_ids,
    route_weights,
    w_gate,
    w_up,
    w_down,
):
    here, heads, _ = query_a.shape
    da, db = query_a.shape[2] // 2, query_b.shape[2] // 2
    va, vb = value_a.shape[2], value_b.shape[2]
    rows, width = residual.shape
    experts_here, _, hidden = w_gate.shape
    experts_all = experts_here * n_sp
    nz = n_tp // 2
    bf16, f32 = jnp.bfloat16, jnp.float32

    def flat(*arrays):
        return jnp.concatenate([a.reshape(here, -1) for a in arrays], axis=1)

    kv = flat(key_a, value_a, key_b, value_b)
    queries = flat(query_a, query_b)
    chosen = route_ids[:, :, None] == jnp.arange(experts_all, dtype=jnp.int32)
    dense = jnp.sum(jnp.where(chosen, route_weights[:, :, None], 0.0), axis=1)
    lanes = -(-2 * experts_all // 128) * 128
    route = jnp.concatenate(
        [dense, dense, jnp.zeros((rows, lanes - 2 * experts_all), f32)], axis=1
    )
    vmem = pl.BlockSpec(memory_space=pltpu.VMEM)
    hbm = pl.BlockSpec(memory_space=pl.ANY)
    sem = pltpu.SemaphoreType.DMA
    pairs = [(6,), (nz,), (nz - 1,), (nz - 1,), (n_sp - 1, nz), (n_sp, nz), (nz,)]
    pairs += [(n_sp - 1, nz), (nz - 1,)]
    scratch = [
        pltpu.VMEM((n_sp,) + kv.shape, bf16),
        pltpu.VMEM(out_a.shape, bf16),
        pltpu.VMEM(out_b.shape, bf16),
        pltpu.VMEM(w_gate.shape, bf16),
        pltpu.VMEM(w_up.shape, bf16),
        pltpu.VMEM(w_down.shape, bf16),
        pltpu.VMEM((here, heads * va), bf16),
        pltpu.VMEM((here, heads * vb), bf16),
        pltpu.VMEM((2, nz, rows, width), bf16),
        pltpu.VMEM((nz, rows, width), bf16),
        pltpu.VMEM((nz, rows, width), bf16),
        pltpu.VMEM((nz - 1, rows, width), bf16),
        pltpu.VMEM((rows, width), bf16),
        pltpu.VMEM((nz, n_sp, 2, rows, width + lanes), bf16),
        pltpu.VMEM((n_sp * 2 * rows, experts_here * hidden), bf16),
        pltpu.VMEM((nz, 2, n_sp, rows, width), bf16),
        pltpu.VMEM((nz, n_sp, rows, width), bf16),
        pltpu.VMEM((nz, n_sp, rows, width), bf16),
        pltpu.VMEM((n_sp - 1, nz, rows, width), bf16),
        pltpu.VMEM((nz - 1, rows, width), bf16),
        pltpu.VMEM((nz - 1, rows, width), bf16),
        pltpu.VMEM((rows, width), f32),
        sem((6,)),
    ]
    for shape in pairs:
        scratch += [sem(shape), sem(shape)]
    return pl.pallas_call(
        functools.partial(layer_kernel, (n_sp, n_tp, heads, da, db, va, vb)),
        out_shape=jax.ShapeDtypeStruct((rows, width), bf16),
        in_specs=[vmem, vmem, pl.BlockSpec(memory_space=pltpu.SMEM)] + [vmem] * 5 + [hbm] * 5,
        out_specs=vmem,
        scratch_shapes=scratch,
        compiler_params=pltpu.CompilerParams(
            collective_id=0, has_side_effects=True, vmem_limit_bytes=60 * 1024 * 1024
        ),
    )(
        kv,
        queries,
        lambdas,
        gain_a.reshape(1, -1),
        gain_b.reshape(1, -1),
        residual,
        norm_gain.reshape(1, -1),
        route,
        out_a,
        out_b,
        w_gate,
        w_up,
        w_down,
    )


def solution(mesh):
    in_specs = (
        P("sp", "tp", None),
        P("sp", "tp", None),
        P("sp", "tp", None),
        P("sp", "tp", None),
        P("sp", "tp", None),
        P("sp", "tp", None),
        P(None, "tp"),
        P(),
        P(),
        P("tp", None),
        P("tp", None),
        P(("sp", "tp"), None),
        P(),
        P(("sp", "tp"), None),
        P(("sp", "tp"), None),
        P("sp", None, "tp"),
        P("sp", None, "tp"),
        P("sp", "tp", None),
    )
    out_specs = P(("sp", "tp"), None)
    n_sp, n_tp = mesh.shape["sp"], mesh.shape["tp"]
    fits = n_sp == 4 and n_tp % 2 == 0 and n_tp <= 8
    body = functools.partial(per_device, n_sp, n_tp) if fits else per_device_plain
    return jax.shard_map(
        body, mesh=mesh, in_specs=in_specs, out_specs=out_specs, check_vma=False
    )
```
